32 devices in a mesh: ep: 4 (over y, x), tp: 8 (over z, core).
Axes of the slice: x: 2, y: 2, z: 4, core: 2. Of those that a mesh axis runs over, the one named last changes fastest.
Arguments:
- tokens: bfloat16 [896, 4096], P('ep', 'tp'), may hold values from -6 to 6
- picks: int32 [4, 4, 56], P('ep'), may hold values from 0 to 223, as said below
- pick_weights: float32 [4, 4, 56], P('ep'), may hold values from 0.1 to 1
- gate_weight: bfloat16 [4, 1280, 4096], P('ep', 'tp'), may hold values from -0.09375 to 0.09375
- up_weight: bfloat16 [4, 1280, 4096], P('ep', 'tp'), may hold values from -0.09375 to 0.09375
- down_weight: bfloat16 [4, 1280, 4096], P('ep', None, 'tp'), may hold values from -0.15625 to 0.15625
- dense_gate: bfloat16 [5120, 4096], P('tp'), may hold values from -0.09375 to 0.09375
- dense_up: bfloat16 [5120, 4096], P('tp'), may hold values from -0.09375 to 0.09375
- dense_down: bfloat16 [5120, 4096], P('tp'), may hold values from -0.078125 to 0.078125
- branch_gate: float32 [4096], P('tp'), may hold values from -6 to 6
Outputs:
- mixed: bfloat16 [896, 4096], P('ep', 'tp')
The draws below stay inside these ranges and needn't reach their ends.
Inputs may be any that keep to these rules, and one draw needn't show every extreme that they name: For each block s and expert e, the 56 entries picks[s, e, :] are distinct rows of that block.
All inputs are finite; a program needn't handle non-finite values.
Results may differ from the reference program's by a relative error of at most 0.014.
Values may be sent and summed in bfloat16 or wider, within the bound.
A program may use at most 64 MiB of HBM per device.

```python
import jax
import jax.numpy as jnp

D = 4096
FF = 1280
DF = 5120
TOK_DEV = 224
SLOTS = 56
EXPERTS = 4
TOKENS = 896
N_EP = 4
N_TP = 8


def draw_picks(key, part):
    key_list = jax.random.split(key, N_EP * EXPERTS)

    def one_block(subkey):
        return jax.random.permutation(subkey, TOK_DEV)[:SLOTS]
    orders = jax.vmap(one_block)(key_list)
    return orders.reshape(N_EP, EXPERTS, SLOTS).astype(jnp.int32)


def levels(rng, dims, cuts, smallest, high):
    loudness, own = 1.0, jax.random.fold_in(rng, 6)
    for axis_at, shards_of in cuts:
        heights = jnp.exp(jax.random.uniform(jax.random.fold_in(own, axis_at), (shards_of,), jnp.float32, smallest / len(cuts), high / len(cuts)))
        loudness = loudness * jnp.repeat(heights, dims[axis_at] // shards_of).reshape([-1 if axis == axis_at else 1 for axis in range(len(dims))])
    return loudness


def scatter_about(own_key, dims, spread, reach, cuts=(), kind=jnp.bfloat16):
    gain = levels(own_key, dims, cuts, -0.22, 0.18) if cuts else 1.0
    drawn = jax.random.normal(own_key, dims, jnp.float32) * spread * gain
    return jnp.minimum(jnp.maximum(drawn, -reach), reach).astype(kind)


def setup_inputs(seed: int = 0) -> dict:
    streams_of = jax.random.split(jax.random.key(seed), 11)
    tokens = scatter_about(streams_of[0], (TOKENS, D), 1.0, 6.0, ((0, 4), (1, 8)))
    picks = draw_picks(jax.random.fold_in(streams_of[10], 71), 0)
    pick_weights = jnp.clip(0.1 + 0.9 * jax.random.uniform(streams_of[2], (N_EP, EXPERTS, SLOTS), jnp.float32) ** levels(streams_of[2], (N_EP, EXPERTS, SLOTS), ((0, 4),), -0.2, 0.2), 0.1, 1.0)
    gate_weight = scatter_about(streams_of[3], (EXPERTS, FF, D), D ** -0.5, 0.09375, ((0, 4), (1, 8)))
    up_weight = scatter_about(streams_of[4], (EXPERTS, FF, D), D ** -0.5, 0.09375, ((0, 4), (1, 8)))
    down_weight = scatter_about(streams_of[5], (EXPERTS, FF, D), FF ** -0.5, 0.15625, ((0, 4), (2, 8)))
    dense_gate = scatter_about(streams_of[6], (DF, D), D ** -0.5, 0.09375, ((0, 8),))
    dense_up = scatter_about(streams_of[7], (DF, D), D ** -0.5, 0.09375, ((0, 8),))
    dense_down = scatter_about(streams_of[8], (DF, D), DF ** -0.5, 0.078125, ((0, 8),))
    branch_gate = scatter_about(streams_of[9], (D,), 1.5, 6.0, ((0, 8),), jnp.float32)
    return dict(tokens=tokens, picks=picks, pick_weights=pick_weights, gate_weight=gate_weight, up_weight=up_weight, down_weight=down_weight, dense_gate=dense_gate, dense_up=dense_up, dense_down=dense_down, branch_gate=branch_gate)


def reference(tokens, picks, pick_weights, gate_weight, up_weight, down_weight, dense_gate, dense_up, dense_down, branch_gate):
    offsets = (jnp.arange(N_EP, dtype=jnp.int32) * TOK_DEV)[:, None]
    mixture = jnp.zeros((TOKENS, D), jnp.float32)
    for expert in range(EXPERTS):
        row_index = (picks[:, expert, :] + offsets).reshape(-1).astype(jnp.int32)
        chosen = tokens[row_index]
        gate_value = jnp.dot(chosen, gate_weight[expert].T, preferred_element_type=jnp.float32)
        up_value = jnp.dot(chosen, up_weight[expert].T, preferred_element_type=jnp.float32)
        hidden = (jax.nn.silu(gate_value) * up_value).astype(jnp.bfloat16)
        result = jnp.dot(hidden, down_weight[expert], preferred_element_type=jnp.float32).astype(jnp.bfloat16)
        weights = pick_weights[:, expert, :].reshape(-1, 1)
        mixture = mixture.at[row_index].add(result.astype(jnp.float32) * weights)
    dense_gval = jnp.dot(tokens, dense_gate.T, preferred_element_type=jnp.float32)
    dense_uval = jnp.dot(tokens, dense_up.T, preferred_element_type=jnp.float32)
    dense_hidden = (jax.nn.silu(dense_gval) * dense_uval).astype(jnp.bfloat16)
    block_width = DF // N_TP
    dense_out = jnp.zeros((TOKENS, D), jnp.float32)
    for block_index in range(N_TP):
        lower = block_index * block_width
        partial_value = jnp.dot(dense_hidden[:, lower:lower + block_width], dense_down[lower:lower + block_width], preferred_element_type=jnp.float32)
        dense_out = dense_out + partial_value.astype(jnp.bfloat16).astype(jnp.float32)
    mixed = mixture + jax.nn.sigmoid(branch_gate)[None, :] * dense_out
    return mixed.astype(jnp.bfloat16)
```

```python
import functools

import jax
import jax.numpy as jnp
from jax import lax
from jax.experimental import pallas as pl
from jax.experimental.pallas import tpu as pltpu
from jax.sharding import PartitionSpec as P

MESH = pl.DeviceIdType.MESH
BF = jnp.bfloat16
F32 = jnp.float32
CORES = 2
G = 2
NT = (((1,), (1,)), ((), ()))
NN = (((1,), (0,)), ((), ()))


def mm(a, b, dims=NN):
    return lax.dot_general(a, b, dims, preferred_element_type=F32)


def silu(v):
    return v / (1.0 + jnp.exp(-v))


def kernel(
    n_ep, n_tp, pad,
    tok_hbm, pcol, prow, pw, weg_hbm, weu_hbm, wed_hbm, wg_hbm, wu_hbm, wd_hbm, bg,
    out_ref,
    x, wg, wu, wd, weg, weu, wed, acc_g, acc_u, oh, pk, ch, acc_eg, acc_eu,
    hx, acc_o, eo, back, hd, ps, pr, own, ru, rd, su, sd, acc_d,
    w_sem, ag_recv, ag_up, ag_dn, ag_pt, c_recv, c_send, cf_recv, cf_send,
    h_recv, h_send, hf_recv, hf_send, e_recv, e_send, p_recv, p_send,
    ru_recv, ru_send, rd_recv, rd_send,
):
    nz = n_tp // CORES
    rows, dl = x.shape[1], x.shape[2]
    rh = rows // G
    s = lax.axis_index("ep")
    t = lax.axis_index("tp")
    z = t // CORES
    c = t % CORES
    partner = CORES * z + (1 - c)

    loads = [
        pltpu.make_async_copy(src, dst, w_sem.at[i])
        for i, (src, dst) in enumerate(
            [(tok_hbm, x.at[t]), (wg_hbm, wg), (wu_hbm, wu), (weg_hbm, weg),
             (weu_hbm, weu), (wd_hbm, wd), (wed_hbm, wed)]
        )
    ]
    for cp in loads:
        cp.start()

    barrier = pltpu.get_barrier_semaphore()
    pl.semaphore_signal(barrier, inc=1, device_id={"tp": partner}, device_id_type=MESH)
    for k in range(1, nz):
        pl.semaphore_signal(
            barrier, inc=1, device_id={"tp": CORES * ((z + k) % nz) + c}, device_id_type=MESH
        )
    for k in range(1, n_ep):
        pl.semaphore_signal(barrier, inc=1, device_id={"ep": (s + k) % n_ep}, device_id_type=MESH)

    oh[...] = (
        lax.broadcasted_iota(jnp.int32, oh.shape, 1) == pcol[...]
    ).astype(F32).astype(BF)
    acc_g[...] = jnp.zeros_like(acc_g)
    acc_u[...] = jnp.zeros_like(acc_u)
    acc_eg[...] = jnp.zeros_like(acc_eg)
    acc_eu[...] = jnp.zeros_like(acc_eu)
    acc_o[...] = jnp.zeros_like(acc_o)

    def remote(src, dst, ssem, rsem, **dev):
        return pltpu.make_async_remote_copy(
            src_ref=src, dst_ref=dst, send_sem=ssem, recv_sem=rsem,
            device_id=dev, device_id_type=MESH,
        )

    def part(g):
        return pl.ds(g * rh, rh)

    up_dev = jnp.minimum(t + CORES, n_tp - CORES + c)
    dn_dev = jnp.maximum(t - CORES, c)

    def ag_copy(zi, g, ssem, dev):
        j = CORES * zi + c
        ref = x.at[j, part(g), :]
        return remote(ref, ref, ssem.at[zi, g], ag_recv.at[j, g], tp=dev)

    def ag_wait(j, g):
        ref = x.at[j, part(g), :]
        remote(ref, ref, ag_pt.at[0, 0], ag_recv.at[j, g], tp=partner).wait_recv()

    def c_copy(zi, e, src_rows, dst_rows, sem_e, rsem_e):
        j = CORES * zi + c
        return remote(
            pk.at[zi, pl.ds(pl.multiple_of(src_rows, pad), pad), :],
            ch.at[j, pl.ds(pl.multiple_of(dst_rows, pad), pad), :],
            c_send.at[zi, sem_e], c_recv.at[zi, rsem_e], ep=e,
        )

    def cf_copy(zi, core):
        ref = ch.at[CORES * zi + core]
        return remote(ref, ref, cf_send.at[zi], cf_recv.at[zi], tp=partner)

    def cols(j):
        return pl.ds(pl.multiple_of(j * dl, dl), dl)

    def order(i):
        d = (i + 1) // 2
        return z + (1 - 2 * (i % 2)) * d

    steps = 2 * nz - 1

    loads[0].wait()
    pl.semaphore_wait(barrier, 1 + (nz - 1) + (n_ep - 1))

    def forward(zi):
        for g in range(G):
            @pl.when(zi != z)
            def _():
                ag_wait(CORES * zi + c, g)

            @pl.when((zi <= z) & (z < nz - 1))
            def _():
                ag_copy(zi, g, ag_up, up_dev).start()

            @pl.when((zi >= z) & (z > 0))
            def _():
                ag_copy(zi, g, ag_dn, dn_dev).start()

            ag_copy(zi, g, ag_pt, partner).start()

    forward(z)
    loads[1].wait()
    loads[2].wait()

    @pl.loop(0, steps)
    def _(i):
        zi = order(i)

        @pl.when((zi >= 0) & (zi < nz))
        def _():
            @pl.when(zi != z)
            def _():
                forward(zi)

            mine = CORES * zi + c
            pk[zi] = mm(oh[...], x[mine]).astype(BF)
            for k in range(1, n_ep):
                e = (s + k) % n_ep
                c_copy(zi, e, e * pad, s * pad, e, s).start()
            keep = pl.ds(pl.multiple_of(s * pad, pad), pad)
            ch[mine, keep, :] = pk[zi, keep, :]

            @pl.loop(0, CORES)
            def _(q):
                j = CORES * zi + (c + q) % CORES

                @pl.when(q > 0)
                def _():
                    for g in range(G):
                        ag_wait(j, g)

                acc_g[...] += mm(x[j], wg[:, cols(j)], NT)
                acc_u[...] += mm(x[j], wu[:, cols(j)], NT)

    hd[...] = (silu(acc_g[...]) * acc_u[...]).astype(BF)
    loads[5].wait()

    def p_copy(zi):
        return remote(ps.at[zi], pr.at[zi], p_send.at[zi], p_recv.at[zi], tp=partner)

    @pl.loop(0, nz)
    def _(zi):
        ps[zi] = mm(hd[...], wd[:, cols(CORES * zi + (1 - c))]).astype(BF)
        p_copy(zi).start()

    @pl.loop(0, nz)
    def _(zi):
        own[zi] = mm(hd[...], wd[:, cols(CORES * zi + c)]).astype(BF)
        p_copy(zi).wait_recv()
        own[zi] = (own[zi].astype(F32) + pr[zi].astype(F32)).astype(BF)

    def rs_up(zu, g, src):
        return remote(src.at[zu, part(g), :], ru.at[zu, part(g), :],
                      ru_send.at[zu, g], ru_recv.at[zu, g], tp=up_dev)

    def rs_dn(zd, g, src):
        return remote(src.at[zd, part(g), :], rd.at[zd, part(g), :],
                      rd_send.at[zd, g], rd_recv.at[zd, g], tp=dn_dev)

    @pl.when(z == 0)
    def _():
        @pl.loop(0, nz - 1)
        def _(i):
            for g in range(G):
                rs_up(nz - 1 - i, g, own).start()

    @pl.when(z == nz - 1)
    def _():
        @pl.loop(0, nz - 1)
        def _(i):
            for g in range(G):
                rs_dn(i, g, own).start()

    loads[3].wait()
    loads[4].wait()

    @pl.loop(0, steps)
    def _(i):
        zi = order(i)

        @pl.when((zi >= 0) & (zi < nz))
        def _():
            for k in range(1, n_ep):
                e = (s + k) % n_ep
                c_copy(zi, e, e * pad, e * pad, e, e).wait_recv()
            cf_copy(zi, c).start()

            @pl.loop(0, CORES)
            def _(q):
                j = CORES * zi + (c + q) % CORES

                @pl.when(q > 0)
                def _():
                    cf_copy(zi, 1 - c).wait_recv()

                acc_eg[...] += mm(ch[j], weg[:, cols(j)], NT)
                acc_eu[...] += mm(ch[j], weu[:, cols(j)], NT)

    hx[t] = (silu(acc_eg[...]) * acc_eu[...]).astype(BF)

    def h_copy(zo, src_z, sidx):
        ref = hx.at[CORES * src_z + c]
        return remote(ref, ref, h_send.at[sidx], h_recv.at[src_z], tp=CORES * zo + c)

    def hf_copy(zi, core):
        ref = hx.at[CORES * zi + core]
        return remote(ref, ref, hf_send.at[zi], hf_recv.at[zi], tp=partner)

    for k in range(1, nz):
        zo = (z + k) % nz
        h_copy(zo, z, zo).start()
    hf_copy(z, c).start()

    @pl.when((z > 0) & (z < nz - 1))
    def _():
        @pl.loop(0, nz - 1)
        def _(i):
            zu = nz - 1 - i
            zd = i
            for g in range(G):
                @pl.when(zu > z)
                def _():
                    rs_up(zu, g, su).wait_recv()
                    su[zu, part(g), :] = (
                        own[zu, part(g), :].astype(F32) + ru[zu, part(g), :].astype(F32)
                    ).astype(BF)
                    rs_up(zu, g, su).start()

                @pl.when(zd < z)
                def _():
                    rs_dn(zd, g, sd).wait_recv()
                    sd[zd, part(g), :] = (
                        own[zd, part(g), :].astype(F32) + rd[zd, part(g), :].astype(F32)
                    ).astype(BF)
                    rs_dn(zd, g, sd).start()

    loads[6].wait()

    @pl.loop(0, steps)
    def _(i):
        zi = order(i)

        @pl.when((zi >= 0) & (zi < nz))
        def _():
            @pl.when(zi != z)
            def _():
                h_copy((z + 1) % nz, zi, z).wait_recv()
                hf_copy(zi, c).start()

            @pl.loop(0, CORES)
            def _(q):
                j = CORES * zi + (c + q) % CORES

                @pl.when(q > 0)
                def _():
                    hf_copy(zi, 1 - c).wait_recv()

                acc_o[...] += mm(hx[j], wed[j])

    eo[...] = acc_o[...].astype(BF)

    def e_copy(dev, src_i, dst_i, ssem, rsem):
        return remote(
            eo.at[pl.ds(pl.multiple_of(src_i * pad, pad), pad), :],
            back.at[pl.ds(pl.multiple_of(dst_i * pad, pad), pad), :],
            e_send.at[ssem], e_recv.at[rsem], ep=dev,
        )

    for k in range(1, n_ep):
        e = (s + k) % n_ep
        e_copy(e, e, s, e, s).start()
    keep = pl.ds(pl.multiple_of(s * pad, pad), pad)
    back[keep, :] = eo[keep, :]

    acc_d[...] = own[z].astype(F32)

    @pl.when(z > 0)
    def _():
        for g in range(G):
            rs_up(z, g, su).wait_recv()
            acc_d[part(g), :] += ru[z, part(g), :].astype(F32)

    @pl.when(z < nz - 1)
    def _():
        for g in range(G):
            rs_dn(z, g, sd).wait_recv()
            acc_d[part(g), :] += rd[z, part(g), :].astype(F32)

    match = lax.broadcasted_iota(jnp.int32, (rows, prow.shape[1]), 0) == prow[...]
    sel = jnp.where(match, pw[...], 0.0)
    hi = sel.astype(BF)
    lo = (sel - hi.astype(F32)).astype(BF)
    acc_d[...] = acc_d[...] * (1.0 / (1.0 + jnp.exp(-bg[...])))
    for k in range(1, n_ep):
        e = (s + k) % n_ep
        e_copy(e, e, e, e, e).wait_recv()
    out_ref[...] = (acc_d[...] + mm(hi, back[...]) + mm(lo, back[...])).astype(BF)

    @pl.loop(0, nz)
    def _(zi):
        for g in range(G):
            @pl.when((zi <= z) & (z < nz - 1))
            def _():
                ag_copy(zi, g, ag_up, up_dev).wait_send()

            @pl.when((zi >= z) & (z > 0))
            def _():
                ag_copy(zi, g, ag_dn, dn_dev).wait_send()

            ag_copy(zi, g, ag_pt, partner).wait_send()

            @pl.when(zi > z)
            def _():
                rs_up(zi, g, su).wait_send()

            @pl.when(zi < z)
            def _():
                rs_dn(zi, g, sd).wait_send()

        for k in range(1, n_ep):
            e = (s + k) % n_ep
            c_copy(zi, e, e * pad, s * pad, e, s).wait_send()
        cf_copy(zi, c).wait_send()
        p_copy(zi).wait_send()
        hf_copy(zi, c).wait_send()

        @pl.when(zi != z)
        def _():
            h_copy((z + 1) % nz, z, zi).wait_send()

    for k in range(1, n_ep):
        e = (s + k) % n_ep
        e_copy(e, e, s, e, s).wait_send()


def per_device(
    n_ep, n_tp, tokens, picks, pick_weights, gate_weight, up_weight, down_weight,
    dense_gate, dense_up, dense_down, branch_gate,
):
    rows, dl = tokens.shape
    slots = picks.shape[2]
    pad = -(-slots // 16) * 16
    nz = n_tp // CORES
    he, width = gate_weight.shape[1], gate_weight.shape[2]
    hd = dense_gate.shape[0]
    ep_rows = n_ep * pad
    fill = ((0, 0), (0, pad - slots))
    padded = jnp.pad(picks[0], fill, constant_values=-1)
    weights = jnp.pad(pick_weights[0], fill)
    vm = pl.BlockSpec(memory_space=pltpu.VMEM)
    hbm = pl.BlockSpec(memory_space=pl.ANY)
    sem = pltpu.SemaphoreType.DMA
    blocks = pltpu.VMEM((nz, rows, dl), BF)
    return pl.pallas_call(
        functools.partial(kernel, n_ep, n_tp, pad),
        out_shape=jax.ShapeDtypeStruct((rows, dl), BF),
        in_specs=[hbm, vm, vm, vm, hbm, hbm, hbm, hbm, hbm, hbm, vm],
        out_specs=vm,
        scratch_shapes=[
            pltpu.VMEM((n_tp, rows, dl), BF),
            pltpu.VMEM((hd, width), BF),
            pltpu.VMEM((hd, width), BF),
            pltpu.VMEM((hd, width), BF),
            pltpu.VMEM((he, width), BF),
            pltpu.VMEM((he, width), BF),
            pltpu.VMEM((n_tp, he, dl), BF),
            pltpu.VMEM((rows, hd), F32),
            pltpu.VMEM((rows, hd), F32),
            pltpu.VMEM((ep_rows, rows), BF),
            pltpu.VMEM((nz, ep_rows, dl), BF),
            pltpu.VMEM((n_tp, ep_rows, dl), BF),
            pltpu.VMEM((ep_rows, he), F32),
            pltpu.VMEM((ep_rows, he), F32),
            pltpu.VMEM((n_tp, ep_rows, he), BF),
            pltpu.VMEM((ep_rows, dl), F32),
            pltpu.VMEM((ep_rows, dl), BF),
            pltpu.VMEM((ep_rows, dl), BF),
            pltpu.VMEM((rows, hd), BF),
            blocks, blocks, blocks, blocks, blocks, blocks, blocks,
            pltpu.VMEM((rows, dl), F32),
            sem((7,)),
            sem((n_tp, G)), sem((nz, G)), sem((nz, G)), sem((nz, G)),
            sem((nz, n_ep)), sem((nz, n_ep)), sem((nz,)), sem((nz,)),
            sem((nz,)), sem((nz,)), sem((nz,)), sem((nz,)),
            sem((n_ep,)), sem((n_ep,)), sem((nz,)), sem((nz,)),
            sem((nz, G)), sem((nz, G)), sem((nz, G)), sem((nz, G)),
        ],
        compiler_params=pltpu.CompilerParams(
            collective_id=0, has_side_effects=True, vmem_limit_bytes=60 * 1024 * 1024
        ),
    )(
        tokens, padded.reshape(-1, 1), padded.reshape(1, -1), weights.reshape(1, -1),
        gate_weight[0], up_weight[0], down_weight[0].reshape(n_tp, he, dl),
        dense_gate, dense_up, dense_down, branch_gate.reshape(1, -1),
    )


def solution(mesh):
    in_specs = (
        P("ep", "tp"),
        P("ep", None, None),
        P("ep", None, None),
        P("ep", "tp", None),
        P("ep", "tp", None),
        P("ep", None, "tp"),
        P("tp", None),
        P("tp", None),
        P("tp", None),
        P("tp"),
    )
    return jax.shard_map(
        functools.partial(per_device, mesh.shape["ep"], mesh.shape["tp"]),
        mesh=mesh, in_specs=in_specs, out_specs=P("ep", "tp"), check_vma=False,
    )
```

```python
import functools

import jax
import jax.numpy as jnp
from jax import lax
from jax.experimental import pallas as pl
from jax.experimental.pallas import tpu as pltpu
from jax.sharding import PartitionSpec as P

MESH = pl.DeviceIdType.MESH
BF = jnp.bfloat16
F32 = jnp.float32
CORES = 2
G = 2
NT = (((1,), (1,)), ((), ()))
NN = (((1,), (0,)), ((), ()))
TN = (((0,), (0,)), ((), ()))


def mm(a, b, dims=NN):
    return lax.dot_general(a, b, dims, preferred_element_type=F32)


def silu(v):
    return v / (1.0 + jnp.exp(-v))


def kernel(
    n_ep, n_tp, pad,
    tok_hbm, pk_in, pw_in, weg_hbm, weu_hbm, wed_hbm, wg_hbm, wu_hbm, wd_hbm, bg,
    out_ref,
    x, wg, wu, wd, weg, weu, wed, acc_g, acc_u, oh, pk, ch, acc_eg, acc_eu,
    hx, acc_o, eo, back, hd, ps, pr, own, ru, rd, su, sd, acc_d,
    w_sem, ag_recv, ag_up, ag_dn, ag_pt, c_recv, c_send, cf_recv, cf_send,
    h_recv, h_send, hf_recv, hf_send, e_recv, e_send, p_recv, p_send,
    ru_recv, ru_send, rd_recv, rd_send,
):
    nz = n_tp // CORES
    rows, dl = x.shape[1], x.shape[2]
    rh = rows // G
    s = lax.axis_index("ep")
    t = lax.axis_index("tp")
    z = t // CORES
    c = t % CORES
    partner = CORES * z + (1 - c)

    loads = [
        pltpu.make_async_copy(src, dst, w_sem.at[i])
        for i, (src, dst) in enumerate(
            [(tok_hbm, x.at[t]), (wg_hbm, wg), (wu_hbm, wu), (weg_hbm, weg),
             (weu_hbm, weu), (wd_hbm, wd), (wed_hbm, wed)]
        )
    ]
    for cp in loads:
        cp.start()

    barrier = pltpu.get_barrier_semaphore()
    pl.semaphore_signal(barrier, inc=1, device_id={"tp": partner}, device_id_type=MESH)
    for k in range(1, nz):
        pl.semaphore_signal(
            barrier, inc=1, device_id={"tp": CORES * ((z + k) % nz) + c}, device_id_type=MESH
        )
    for k in range(1, n_ep):
        pl.semaphore_signal(barrier, inc=1, device_id={"ep": (s + k) % n_ep}, device_id_type=MESH)

    slots = pk_in.shape[2]
    spread = (
        lax.broadcasted_iota(jnp.int32, (pad, slots), 0)
        == lax.broadcasted_iota(jnp.int32, (pad, slots), 1)
    ).astype(F32).astype(BF)

    def match(e):
        ids = lax.broadcasted_iota(jnp.int32, (rows, slots), 0)
        return ids == pk_in[0, pl.ds(e, 1), :]

    for e in range(n_ep):
        hot = match(e).astype(F32).astype(BF)
        oh[e * pad:(e + 1) * pad, :] = mm(spread, hot, NT).astype(BF)
    acc_g[...] = jnp.zeros_like(acc_g)
    acc_u[...] = jnp.zeros_like(acc_u)
    acc_eg[...] = jnp.zeros_like(acc_eg)
    acc_eu[...] = jnp.zeros_like(acc_eu)
    acc_o[...] = jnp.zeros_like(acc_o)

    def remote(src, dst, ssem, rsem, **dev):
        return pltpu.make_async_remote_copy(
            src_ref=src, dst_ref=dst, send_sem=ssem, recv_sem=rsem,
            device_id=dev, device_id_type=MESH,
        )

    def part(g):
        return pl.ds(g * rh, rh)

    up_dev = jnp.minimum(t + CORES, n_tp - CORES + c)
    dn_dev = jnp.maximum(t - CORES, c)

    def ag_copy(zi, g, ssem, dev):
        j = CORES * zi + c
        ref = x.at[j, part(g), :]
        return remote(ref, ref, ssem.at[zi, g], ag_recv.at[j, g], tp=dev)

    def ag_wait(j, g):
        ref = x.at[j, part(g), :]
        remote(ref, ref, ag_pt.at[0, 0], ag_recv.at[j, g], tp=partner).wait_recv()

    def c_copy(zi, e, src_rows, dst_rows, sem_e, rsem_e):
        j = CORES * zi + c
        return remote(
            pk.at[zi, pl.ds(pl.multiple_of(src_rows, pad), pad), :],
            ch.at[j, pl.ds(pl.multiple_of(dst_rows, pad), pad), :],
            c_send.at[zi, sem_e], c_recv.at[zi, rsem_e], ep=e,
        )

    def cf_copy(zi, core):
        ref = ch.at[CORES * zi + core]
        return remote(ref, ref, cf_send.at[zi], cf_recv.at[zi], tp=partner)

    def cols(j):
        return pl.ds(pl.multiple_of(j * dl, dl), dl)

    near = jnp.minimum(z, nz - 1 - z)

    def order(m):
        both = z + (1 - 2 * (m % 2)) * ((m + 1) // 2)
        far = jnp.where(2 * z < nz - 1, z + m - near, z - m + near)
        return jnp.where(m <= 2 * near, both, far)

    loads[0].wait()
    pl.semaphore_wait(barrier, 1 + (nz - 1) + (n_ep - 1))

    def forward(zi):
        for g in range(G):
            @pl.when(zi != z)
            def _():
                ag_wait(CORES * zi + c, g)

            @pl.when((zi <= z) & (z < nz - 1))
            def _():
                ag_copy(zi, g, ag_up, up_dev).start()

            @pl.when((zi >= z) & (z > 0))
            def _():
                ag_copy(zi, g, ag_dn, dn_dev).start()

            ag_copy(zi, g, ag_pt, partner).start()

    forward(z)

    def dense_block(j):
        acc_g[...] += mm(x[j], wg[:, cols(j)], NT)
        acc_u[...] += mm(x[j], wu[:, cols(j)], NT)

    @pl.loop(0, nz)
    def _(m):
        zi = order(m)
        mine = CORES * zi + c
        pk[zi] = mm(oh[...], x[mine]).astype(BF)
        for k in range(1, n_ep):
            e = (s + k) % n_ep
            c_copy(zi, e, e * pad, s * pad, e, s).start()
        keep = pl.ds(pl.multiple_of(s * pad, pad), pad)
        ch[mine, keep, :] = pk[zi, keep, :]

        @pl.when(m == 0)
        def _():
            loads[1].wait()
            loads[2].wait()

        dense_block(mine)

        @pl.when(m < nz - 1)
        def _():
            forward(order(m + 1))

        other = CORES * zi + (1 - c)
        for g in range(G):
            ag_wait(other, g)
        dense_block(other)

    hd[...] = (silu(acc_g[...]) * acc_u[...]).astype(BF)
    loads[5].wait()

    def p_copy(zi):
        return remote(ps.at[zi], pr.at[zi], p_send.at[zi], p_recv.at[zi], tp=partner)

    @pl.loop(0, nz)
    def _(zi):
        ps[zi] = mm(hd[...], wd[:, cols(CORES * zi + (1 - c))]).astype(BF)
        p_copy(zi).start()

    @pl.loop(0, nz)
    def _(zi):
        own[zi] = mm(hd[...], wd[:, cols(CORES * zi + c)]).astype(BF)
        p_copy(zi).wait_recv()
        own[zi] = (own[zi].astype(F32) + pr[zi].astype(F32)).astype(BF)

    def rs_up(zu, g, src):
        return remote(src.at[zu, part(g), :], ru.at[zu, part(g), :],
                      ru_send.at[zu, g], ru_recv.at[zu, g], tp=up_dev)

    def rs_dn(zd, g, src):
        return remote(src.at[zd, part(g), :], rd.at[zd, part(g), :],
                      rd_send.at[zd, g], rd_recv.at[zd, g], tp=dn_dev)

    @pl.when(z == 0)
    def _():
        @pl.loop(0, nz - 1)
        def _(i):
            for g in range(G):
                rs_up(nz - 1 - i, g, own).start()

    @pl.when(z == nz - 1)
    def _():
        @pl.loop(0, nz - 1)
        def _(i):
            for g in range(G):
                rs_dn(i, g, own).start()

    loads[3].wait()
    loads[4].wait()

    @pl.loop(0, nz)
    def _(m):
        zi = order(m)
        for k in range(1, n_ep):
            e = (s + k) % n_ep
            c_copy(zi, e, e * pad, e * pad, e, e).wait_recv()
        cf_copy(zi, c).start()

        @pl.loop(0, CORES)
        def _(q):
            j = CORES * zi + (c + q) % CORES

            @pl.when(q > 0)
            def _():
                cf_copy(zi, 1 - c).wait_recv()

            acc_eg[...] += mm(weg[:, cols(j)], ch[j], NT)
            acc_eu[...] += mm(weu[:, cols(j)], ch[j], NT)

    hx[t] = (silu(acc_eg[...]) * acc_eu[...]).astype(BF)

    def h_copy(zo, src_z, sidx):
        ref = hx.at[CORES * src_z + c]
        return remote(ref, ref, h_send.at[sidx], h_recv.at[src_z], tp=CORES * zo + c)

    def hf_copy(zi, core):
        ref = hx.at[CORES * zi + core]
        return remote(ref, ref, hf_send.at[zi], hf_recv.at[zi], tp=partner)

    for k in range(1, nz):
        zo = (z + k) % nz
        h_copy(zo, z, zo).start()
    hf_copy(z, c).start()

    @pl.when((z > 0) & (z < nz - 1))
    def _():
        @pl.loop(0, nz - 1)
        def _(i):
            zu = nz - 1 - i
            zd = i
            for g in range(G):
                @pl.when(zu > z)
                def _():
                    rs_up(zu, g, su).wait_recv()
                    su[zu, part(g), :] = (
                        own[zu, part(g), :].astype(F32) + ru[zu, part(g), :].astype(F32)
                    ).astype(BF)
                    rs_up(zu, g, su).start()

                @pl.when(zd < z)
                def _():
                    rs_dn(zd, g, sd).wait_recv()
                    sd[zd, part(g), :] = (
                        own[zd, part(g), :].astype(F32) + rd[zd, part(g), :].astype(F32)
                    ).astype(BF)
                    rs_dn(zd, g, sd).start()

    loads[6].wait()

    @pl.loop(0, nz)
    def _(m):
        zi = order(m)
        @pl.when(zi != z)
        def _():
            h_copy((z + 1) % nz, zi, z).wait_recv()
            hf_copy(zi, c).start()

        @pl.loop(0, CORES)
        def _(q):
            j = CORES * zi + (c + q) % CORES

            @pl.when(q > 0)
            def _():
                hf_copy(zi, 1 - c).wait_recv()

            acc_o[...] += mm(hx[j], wed[j], TN)

    eo[...] = acc_o[...].astype(BF)

    def e_copy(dev, src_i, dst_i, ssem, rsem):
        return remote(
            eo.at[pl.ds(pl.multiple_of(src_i * pad, pad), pad), :],
            back.at[pl.ds(pl.multiple_of(dst_i * pad, pad), pad), :],
            e_send.at[ssem], e_recv.at[rsem], ep=dev,
        )

    for k in range(1, n_ep):
        e = (s + k) % n_ep
        e_copy(e, e, s, e, s).start()
    keep = pl.ds(pl.multiple_of(s * pad, pad), pad)
    back[keep, :] = eo[keep, :]

    acc_d[...] = own[z].astype(F32)

    @pl.when(z > 0)
    def _():
        for g in range(G):
            rs_up(z, g, su).wait_recv()
            acc_d[part(g), :] += ru[z, part(g), :].astype(F32)

    @pl.when(z < nz - 1)
    def _():
        for g in range(G):
            rs_dn(z, g, sd).wait_recv()
            acc_d[part(g), :] += rd[z, part(g), :].astype(F32)

    acc_d[...] = acc_d[...] * (1.0 / (1.0 + jnp.exp(-bg[...])))
    for k in range(1, n_ep):
        e = (s + k) % n_ep
        e_copy(e, e, e, e, e).wait_recv()
    for e in range(n_ep):
        sel = jnp.where(match(e), pw_in[0, pl.ds(e, 1), :], 0.0)
        hi = sel.astype(BF)
        lo = (sel - hi.astype(F32)).astype(BF)
        got = back[e * pad:(e + 1) * pad, :]
        acc_d[...] += mm(mm(hi, spread, NT).astype(BF), got) + mm(mm(lo, spread, NT).astype(BF), got)
    out_ref[...] = acc_d[...].astype(BF)

    @pl.loop(0, nz)
    def _(zi):
        for g in range(G):
            @pl.when((zi <= z) & (z < nz - 1))
            def _():
                ag_copy(zi, g, ag_up, up_dev).wait_send()

            @pl.when((zi >= z) & (z > 0))
            def _():
                ag_copy(zi, g, ag_dn, dn_dev).wait_send()

            ag_copy(zi, g, ag_pt, partner).wait_send()

            @pl.when(zi > z)
            def _():
                rs_up(zi, g, su).wait_send()

            @pl.when(zi < z)
            def _():
                rs_dn(zi, g, sd).wait_send()

        for k in range(1, n_ep):
            e = (s + k) % n_ep
            c_copy(zi, e, e * pad, s * pad, e, s).wait_send()
        cf_copy(zi, c).wait_send()
        p_copy(zi).wait_send()
        hf_copy(zi, c).wait_send()

        @pl.when(zi != z)
        def _():
            h_copy((z + 1) % nz, z, zi).wait_send()

    for k in range(1, n_ep):
        e = (s + k) % n_ep
        e_copy(e, e, s, e, s).wait_send()


def per_device(
    n_ep, n_tp, tokens, picks, pick_weights, gate_weight, up_weight, down_weight,
    dense_gate, dense_up, dense_down, branch_gate,
):
    rows, dl = tokens.shape
    slots = picks.shape[2]
    pad = -(-slots // 16) * 16
    nz = n_tp // CORES
    he, width = gate_weight.shape[1], gate_weight.shape[2]
    hd = dense_gate.shape[0]
    ep_rows = n_ep * pad
    vm = pl.BlockSpec(memory_space=pltpu.VMEM)
    hbm = pl.BlockSpec(memory_space=pl.ANY)
    sem = pltpu.SemaphoreType.DMA
    blocks = pltpu.VMEM((nz, rows, dl), BF)
    return pl.pallas_call(
        functools.partial(kernel, n_ep, n_tp, pad),
        out_shape=jax.ShapeDtypeStruct((rows, dl), BF),
        in_specs=[hbm, vm, vm, hbm, hbm, hbm, hbm, hbm, hbm, vm],
        out_specs=vm,
        scratch_shapes=[
            pltpu.VMEM((n_tp, rows, dl), BF),
            pltpu.VMEM((hd, width), BF),
            pltpu.VMEM((hd, width), BF),
            pltpu.VMEM((hd, width), BF),
            pltpu.VMEM((he, width), BF),
            pltpu.VMEM((he, width), BF),
            pltpu.VMEM((n_tp, he, dl), BF),
            pltpu.VMEM((rows, hd), F32),
            pltpu.VMEM((rows, hd), F32),
            pltpu.VMEM((ep_rows, rows), BF),
            pltpu.VMEM((nz, ep_rows, dl), BF),
            pltpu.VMEM((n_tp, ep_rows, dl), BF),
            pltpu.VMEM((he, ep_rows), F32),
            pltpu.VMEM((he, ep_rows), F32),
            pltpu.VMEM((n_tp, he, ep_rows), BF),
            pltpu.VMEM((ep_rows, dl), F32),
            pltpu.VMEM((ep_rows, dl), BF),
            pltpu.VMEM((ep_rows, dl), BF),
            pltpu.VMEM((rows, hd), BF),
            blocks, blocks, blocks, blocks, blocks, blocks, blocks,
            pltpu.VMEM((rows, dl), F32),
            sem((7,)),
            sem((n_tp, G)), sem((nz, G)), sem((nz, G)), sem((nz, G)),
            sem((nz, n_ep)), sem((nz, n_ep)), sem((nz,)), sem((nz,)),
            sem((nz,)), sem((nz,)), sem((nz,)), sem((nz,)),
            sem((n_ep,)), sem((n_ep,)), sem((nz,)), sem((nz,)),
            sem((nz, G)), sem((nz, G)), sem((nz, G)), sem((nz, G)),
        ],
        compiler_params=pltpu.CompilerParams(
            collective_id=0, has_side_effects=True, vmem_limit_bytes=60 * 1024 * 1024
        ),
    )(
        tokens, picks, pick_weights,
        gate_weight[0], up_weight[0], down_weight[0].reshape(n_tp, he, dl),
        dense_gate, dense_up, dense_down, branch_gate.reshape(1, -1),
    )


def solution(mesh):
    in_specs = (
        P("ep", "tp"),
        P("ep", None, None),
        P("ep", None, None),
        P("ep", "tp", None),
        P("ep", "tp", None),
        P("ep", None, "tp"),
        P("tp", None),
        P("tp", None),
        P("tp", None),
        P("tp"),
    )
    return jax.shard_map(
        functools.partial(per_device, mesh.shape["ep"], mesh.shape["tp"]),
        mesh=mesh, in_specs=in_specs, out_specs=P("ep", "tp"), check_vma=False,
    )
```
